32 devices in a mesh: ep: 16 (over z, y, x), tp: 2 (over core).
Axes of the slice: x: 2, y: 2, z: 4, core: 2. Of those that a mesh axis runs over, the one named last changes fastest.
Arguments:
- tokens: bfloat16 [256, 2048], P('ep'), may hold values from -6 to 6
- lengths: int32 [256], P('ep'), may hold values from 1 to 1024
- gain_first: float32 [2048], replicated, may hold values from 0.1 to 1.9
- w_query: bfloat16 [2048, 1024], P(None, 'tp'), may hold values from -0.125 to 0.125
- w_key: bfloat16 [2048, 256], P(None, 'tp'), may hold values from -0.125 to 0.125
- w_value: bfloat16 [2048, 256], P(None, 'tp'), may hold values from -0.125 to 0.125
- cache_keys: bfloat16 [256, 1024, 256], P('ep', None, 'tp'), may hold values from -400 to 400
- cache_values: bfloat16 [256, 1024, 256], P('ep', None, 'tp'), may hold values from -6 to 6
- lambdas: float32 [8], P('tp'), may hold values from 0.3 to 0.8
- head_gain: float32 [8, 128], P('tp'), may hold values from 0.1 to 1.9
- w_output: bfloat16 [1024, 2048], replicated, may hold values from -0.1875 to 0.1875
- gain_second: float32 [2048], replicated, may hold values from 0.1 to 1.9
- w_group: bfloat16 [2048, 4], replicated, may hold values from -0.125 to 0.125
- w_router: bfloat16 [2048, 16], replicated, may hold values from -0.125 to 0.125
- w_blend: bfloat16 [2048], replicated, may hold values from -0.125 to 0.125
- routes: int32 [256, 4], P('ep'), may hold values from 0 to 15, all different within a row; in each aligned block of 16 rows (0 to 15, 16 to 31, ...) at most 8 rows name the same one
- w_expert_gate: bfloat16 [16, 2048, 512], P('ep', None, 'tp'), may hold values from -0.125 to 0.125
- w_expert_up: bfloat16 [16, 2048, 512], P('ep', None, 'tp'), may hold values from -0.125 to 0.125
- w_expert_down: bfloat16 [16, 512, 2048], P('ep', 'tp'), may hold values from -0.25 to 0.25
- w_dense_gate: bfloat16 [2048, 4096], P(None, ('ep', 'tp')), may hold values from -0.125 to 0.125
- w_dense_up: bfloat16 [2048, 4096], P(None, ('ep', 'tp')), may hold values from -0.125 to 0.125
- w_dense_down: bfloat16 [4096, 2048], P(('ep', 'tp')), may hold values from -0.1875 to 0.1875
Outputs:
- layer_out: bfloat16 [256, 2048], P('ep', 'tp')
The draws below stay inside these ranges and needn't reach their ends.
Inputs may be any that keep to these rules, and one draw needn't show every extreme that they name: `routes`: in the rows of one index of ep no expert is named by more than 8 rows, a bound that some block reaches; a row names 4 different experts.
All inputs are finite; a program needn't handle non-finite values.
Results may differ from the reference program's by a relative error of at most 0.012.
The reference program's roundings to bfloat16 on the way count: a program that leaves them out, or rounds other values in their place, can miss the bound.
Values may be sent and summed in bfloat16 or wider, within the bound.
A program may use at most 128 MiB of HBM per device.

```python
import math
import jax
import jax.numpy as jnp
import numpy as np
from jax import lax

D = 2048
HEADS = 8
KVH = 2
HD = 64
VD = 128
FFE = 512
DFF = 4096
N_GROUPS = 4
TOP_K = 4
EXPERTS = 16
SEQ_DEV = 16
CACHE_LEN = 1024
TOKENS = 256
CAP = 8
N_EP = 16


def draw_cache_keys(key, part):
    base = 1.75 * jax.random.normal(key, (TOKENS, CACHE_LEN, KVH * 2 * HD), jnp.float32)
    return jnp.clip(base, -400.0, 400.0).astype(jnp.bfloat16)


def touch_ends(array, stream_key, smallest, largest):
    index_at = [jax.random.randint(jax.random.fold_in(stream_key, axis), (), 0, length) for axis, length in enumerate(array.shape)]
    longest = array.shape.index(max(array.shape))
    next_to = index_at[:longest] + [(index_at[longest] + 1) % array.shape[longest]] + index_at[longest + 1:]
    return array.at[tuple(index_at)].set(smallest).at[tuple(next_to)].set(largest)


def spiked(values, key, source, target, parts, factor):
    owner, partner = [(jnp.arange(values.shape[dim]) // (values.shape[dim] // parts)).reshape([-1 if axis == dim else 1 for axis in range(values.ndim)]) for dim in (source, target)]
    chosen = jax.random.permutation(key, parts)[partner]
    strong = (owner == chosen) | (owner == (partner + parts // 2) % parts)
    return jnp.where(strong, factor * values, values)


def shard_levels(own_key, shape, cuts, low, top_value):
    factor_of = 1.0
    for axis_at, shards_of in cuts:
        draws = jax.random.uniform(jax.random.fold_in(jax.random.fold_in(own_key, 6), axis_at), (shards_of,), jnp.float32, low / len(cuts), top_value / len(cuts))
        factor_of = factor_of * jnp.repeat(jnp.exp(draws), shape[axis_at] // shards_of).reshape((-1,) + (1,) * (len(shape) - 1 - axis_at))
    return factor_of


def deal_out(key, own, number, rows, count, top, most, skew):
    ranking = jax.random.permutation(key, count)
    crowded, ordinary = load_shares(count, rows * top, most, skew, True), load_shares(count, rows * top, most, skew, False)
    places = jnp.arange(count)

    def named(sizes, offset_by):
        used = int((sizes > 0).sum())
        fixed = max(1, used // 4)
        moved = fixed + (places - fixed + offset_by * (used - fixed)) % max(1, count - fixed)
        return jnp.zeros((count,), jnp.int32).at[ranking[jnp.where(places < fixed, places, moved)]].set(jnp.asarray(sizes, jnp.int32))

    sizes = jnp.where(number % 4 == 0, named(crowded, number // 4), named(ordinary, number - number // 4 - 1))
    mixed = jax.random.permutation(jax.random.fold_in(own, 3), count)
    giver, sink = mixed[0:count // 2 * 2:2], mixed[1:count // 2 * 2:2]
    margin = jnp.minimum(sizes[giver] - 1, most - sizes[sink]) // 2
    margin = jnp.where((giver == ranking[0]) | (sink == ranking[0]) | (sizes[sink] == 0), 0, jnp.maximum(margin, 0))
    moved = jax.random.randint(jax.random.fold_in(own, 4), (count // 2,), 0, 1 << 20) % (margin + 1)
    sizes = sizes.at[giver].add(-moved).at[sink].add(moved)
    items = jnp.searchsorted(jnp.cumsum(sizes), jnp.arange(rows * top), side="right").astype(jnp.int32)
    table = items.reshape(top, rows).T
    table = table[jax.random.permutation(jax.random.fold_in(own, 1), rows)]
    offset_by = jax.random.randint(jax.random.fold_in(own, 2), (rows, 1), 0, top)
    return jnp.take_along_axis(table, (jnp.arange(top)[None, :] + offset_by) % top, axis=1)


def load_shares(amount, total, limit, slope, full):
    portions = [(1 << 20) // math.isqrt(grade ** slope) + 1 for grade in range(1, amount + 1)]
    largest = limit if full else min(limit, max(-(-total // amount), total * portions[0] // sum(portions)))
    least = 1 if total - largest >= amount - 1 else 0
    given, spare = [largest] + [least] * (amount - 1), total - largest - least * (amount - 1)
    while spare > 0:
        candidates = [i for i in range(1, amount) if given[i] < largest] or [i for i in range(1, amount) if given[i] < limit]
        pool, budget = sum([portions[i] for i in candidates]), spare
        for i in candidates:
            addition = min(limit - given[i], max(1, budget * portions[i] // pool), spare)
            given[i] = given[i] + addition
            spare = spare - addition
    return np.array(given)


def bell_draw(own_key, shape, scale, bound, pieces=(), kind=jnp.bfloat16):
    array = scale * jax.random.normal(own_key, shape, jnp.float32)
    if pieces:
        array = array * shard_levels(own_key, shape, pieces, -0.22, 0.18)
    return jnp.clip(array, -bound, bound).astype(kind)


def heavy_noise(own_key, extent, scale, reach, cuts, heavy, held_as=jnp.bfloat16):
    values = scale * jax.random.normal(own_key, extent, jnp.float32)
    if cuts:
        values = values * shard_levels(own_key, extent, cuts, -0.22, 0.18)
    return jnp.clip(spiked(values, jax.random.fold_in(own_key, 3), *heavy), -reach, reach).astype(held_as)


def setup_inputs(seed: int = 0) -> dict:
    seeds = jax.random.split(jax.random.key(seed), 23)
    tokens = bell_draw(seeds[0], (TOKENS, D), 1.0, 6.0, ((0, 16),))
    lengths = touch_ends(jax.random.randint(seeds[1], (TOKENS,), 1, CACHE_LEN + 1), jax.random.fold_in(seeds[1], 1), 1, CACHE_LEN).astype(jnp.int32)
    gain_first = jnp.clip(1.0 + 0.18 * jax.random.normal(seeds[2], (D,), jnp.float32), 0.1, 1.9)
    w_query = bell_draw(seeds[3], (D, HEADS * 2 * HD), D ** -0.5, 0.125, ((1, 2),))
    w_key = bell_draw(seeds[4], (D, KVH * 2 * HD), D ** -0.5, 0.125, ((1, 2),))
    w_value = bell_draw(seeds[5], (D, KVH * VD), D ** -0.5, 0.125, ((1, 2),))
    cache_keys = draw_cache_keys(jax.random.fold_in(seeds[22], 71), 0)
    cache_values = bell_draw(seeds[7], (TOKENS, CACHE_LEN, KVH * VD), 1.0, 6.0, ((0, 16), (2, 2)))
    lambdas = jnp.clip(0.3 + 0.5 * jax.random.uniform(seeds[8], (HEADS,), jnp.float32) ** shard_levels(seeds[8], (HEADS,), ((0, 2),), -0.2, 0.2), 0.3, 0.8)
    head_gain = jnp.clip(1.0 + 0.18 * jax.random.normal(seeds[9], (HEADS, VD), jnp.float32), 0.1, 1.9)
    w_output = bell_draw(seeds[10], (HEADS * VD, D), (HEADS * VD) ** -0.5, 0.1875)
    gain_second = jnp.clip(1.0 + 0.18 * jax.random.normal(seeds[11], (D,), jnp.float32), 0.1, 1.9)
    w_group = bell_draw(seeds[12], (D, N_GROUPS), D ** -0.5, 0.125)
    w_router = bell_draw(seeds[13], (D, EXPERTS), D ** -0.5, 0.125)
    w_blend = bell_draw(seeds[14], (D,), D ** -0.5, 0.125)
    routes_keys = jax.random.split(jax.random.fold_in(seeds[15], 1), TOKENS // SEQ_DEV)
    routes_turns = jax.random.permutation(jax.random.fold_in(seeds[15], 3), TOKENS // SEQ_DEV)
    routes = jax.vmap(lambda own, number: deal_out(jax.random.fold_in(seeds[15], 2), own, number, SEQ_DEV, EXPERTS, TOP_K, CAP, 2))(routes_keys, routes_turns).reshape((TOKENS, TOP_K))
    w_expert_gate = bell_draw(seeds[16], (EXPERTS, D, FFE), D ** -0.5, 0.125, ((0, 16), (2, 2)))
    w_expert_up = bell_draw(seeds[17], (EXPERTS, D, FFE), D ** -0.5, 0.125, ((0, 16), (2, 2)))
    w_expert_down = bell_draw(seeds[18], (EXPERTS, FFE, D), FFE ** -0.5, 0.25, ((0, 16), (1, 2)))
    w_dense_gate = bell_draw(seeds[19], (D, DFF), D ** -0.5, 0.125, ((1, 32),))
    w_dense_up = bell_draw(seeds[20], (D, DFF), D ** -0.5, 0.125, ((1, 32),))
    w_dense_down = heavy_noise(seeds[21], (DFF, D), DFF ** -0.5, 0.1875, ((0, 32),), (0, 1, 32, 2.75))
    return {"tokens": tokens, "lengths": lengths, "gain_first": gain_first, "w_query": w_query, "w_key": w_key, "w_value": w_value, "cache_keys": cache_keys, "cache_values": cache_values, "lambdas": lambdas, "head_gain": head_gain, "w_output": w_output, "gain_second": gain_second, "w_group": w_group, "w_router": w_router, "w_blend": w_blend, "routes": routes, "w_expert_gate": w_expert_gate, "w_expert_up": w_expert_up, "w_expert_down": w_expert_down, "w_dense_gate": w_dense_gate, "w_dense_up": w_dense_up, "w_dense_down": w_dense_down}


def layer_norm(values, gain):
    floats = values.astype(jnp.float32)
    center = floats - lax.optimization_barrier(jnp.mean(floats, -1, keepdims=True))
    spread = lax.optimization_barrier(jnp.mean(center * center, -1, keepdims=True))
    return center * lax.rsqrt(spread + 1e-05) * gain

def rotate(values, position):
    half = values.shape[-1] // 2
    inverse = 10000.0 ** (-jnp.arange(half, dtype=jnp.float32) / half)
    angle = position.astype(jnp.float32)[..., None] * inverse
    cosine = jnp.cos(angle)
    sine = jnp.sin(angle)
    first = values[..., :half]
    second = values[..., half:]
    return jnp.concatenate([first * cosine - second * sine, second * cosine + first * sine], -1)

def attend_one(query, key_new, value_new, cache_k, cache_v, length, lam):
    span = cache_k.shape[0]
    scale = HD ** (-0.5)
    keys = cache_k.reshape(span, KVH, 2, HD).astype(jnp.float32)
    scores = jnp.einsum('kgcd,lkcd->kgcl', query.astype(jnp.float32), keys) * scale
    valid = jnp.arange(span) < length
    scores = jnp.where(valid, scores, -jnp.inf)
    own = jnp.einsum('kgcd,kcd->kgc', query.astype(jnp.float32), key_new.astype(jnp.float32)) * scale
    top = jnp.maximum(lax.optimization_barrier(jnp.max(scores, -1)), own)
    expo = jnp.exp(scores - top[..., None])
    own_e = jnp.exp(own - top)
    total = lax.optimization_barrier(jnp.sum(expo, -1)) + own_e
    probs = expo / total[..., None]
    own_p = own_e / total
    weights = (probs[:, :, 0] - lam[..., None] * probs[:, :, 1]).astype(jnp.bfloat16)
    own_w = (own_p[:, :, 0] - lam * own_p[:, :, 1]).astype(jnp.bfloat16)
    values = cache_v.reshape(span, KVH, VD).astype(jnp.float32)
    mixed = jnp.einsum('kgl,lkv->kgv', weights.astype(jnp.float32), values)
    return mixed + own_w.astype(jnp.float32)[..., None] * value_new.astype(jnp.float32)[:, None, :]

def reference(tokens, lengths, gain_first, w_query, w_key, w_value, cache_keys, cache_values, lambdas, head_gain, w_output, gain_second, w_group, w_router, w_blend, routes, w_expert_gate, w_expert_up, w_expert_down, w_dense_gate, w_dense_up, w_dense_down):
    count = tokens.shape[0]
    group = HEADS // KVH
    normed = layer_norm(tokens, gain_first).astype(jnp.bfloat16)
    query = jnp.dot(normed, w_query, preferred_element_type=jnp.float32).reshape(count, KVH, group, 2, HD)
    query = rotate(query, lengths[:, None, None, None]).astype(jnp.bfloat16)
    key_new = jnp.dot(normed, w_key, preferred_element_type=jnp.float32).reshape(count, KVH, 2, HD)
    key_new = rotate(key_new, lengths[:, None, None]).astype(jnp.bfloat16)
    value_new = jnp.dot(normed, w_value, preferred_element_type=jnp.float32).astype(jnp.bfloat16)
    value_new = value_new.reshape(count, KVH, VD)
    lam = lambdas.reshape(KVH, group)
    mixed = lax.map(lambda pack: attend_one(*pack, lam), (query, key_new, value_new, cache_keys, cache_values, lengths))
    mixed = mixed.reshape(count, HEADS, VD)
    heads = mixed * lax.rsqrt(lax.optimization_barrier(jnp.mean(mixed * mixed, -1, keepdims=True)) + 1e-05) * head_gain
    heads = heads.astype(jnp.bfloat16).reshape(count, HEADS * VD)
    resid = tokens.astype(jnp.float32) + jnp.dot(heads, w_output, preferred_element_type=jnp.float32)
    moe_in = layer_norm(resid, gain_second).astype(jnp.bfloat16)
    group_probs = jax.nn.softmax(jnp.dot(moe_in, w_group, preferred_element_type=jnp.float32), -1)
    expert_logits = jnp.dot(moe_in, w_router, preferred_element_type=jnp.float32)
    per_group = EXPERTS // N_GROUPS
    chosen = jnp.take_along_axis(expert_logits, routes, 1)
    group_part = jnp.take_along_axis(group_probs, routes // per_group, 1)
    route_weight = (group_part * jax.nn.softmax(chosen, -1)).astype(jnp.bfloat16)
    blend = jax.nn.sigmoid(jnp.dot(moe_in, w_blend, preferred_element_type=jnp.float32)).astype(jnp.bfloat16)
    dense_gate = jnp.dot(moe_in, w_dense_gate, preferred_element_type=jnp.float32)
    dense_up = jnp.dot(moe_in, w_dense_up, preferred_element_type=jnp.float32)
    dense_hidden = (blend.astype(jnp.float32)[:, None] * jax.nn.silu(dense_gate) * dense_up).astype(jnp.bfloat16)
    dense_out = jnp.dot(dense_hidden, w_dense_down, preferred_element_type=jnp.float32)
    slots = N_EP * CAP

    def expert_step(carry, pack):
        gate_w, up_w, down_w, expert = pack
        match = routes == expert
        weight = lax.optimization_barrier(jnp.sum(jnp.where(match, route_weight.astype(jnp.float32), 0.0), 1))
        hit = jnp.any(match, 1)
        index = jnp.nonzero(hit, size=slots, fill_value=0)[0].astype(jnp.int32)
        live = (jnp.arange(slots) < jnp.sum(hit.astype(jnp.int32))).astype(jnp.float32)
        picked = moe_in[index]
        hidden = (jax.nn.silu(jnp.dot(picked, gate_w, preferred_element_type=jnp.float32)) * jnp.dot(picked, up_w, preferred_element_type=jnp.float32)).astype(jnp.bfloat16)
        result = jnp.dot(hidden, down_w, preferred_element_type=jnp.float32)
        result = result * (weight[index] * live)[:, None]
        return (carry.at[index].add(result), None)
    experts_out, _ = lax.scan(expert_step, jnp.zeros((count, D), jnp.float32), (w_expert_gate, w_expert_up, w_expert_down, jnp.arange(EXPERTS, dtype=jnp.int32)))
    return (resid + dense_out + experts_out).astype(jnp.bfloat16)
```

```python
import functools

import jax
import jax.numpy as jnp
from jax import lax
from jax.experimental import pallas as pl
from jax.experimental.pallas import tpu as pltpu
from jax.sharding import PartitionSpec as P

HD = 64
VD = 128
N_GROUPS = 4


def norm(floats, gain):
    center = floats - jnp.mean(floats, -1, keepdims=True)
    spread = jnp.mean(center * center, -1, keepdims=True)
    return center * lax.rsqrt(spread + 1e-05) * gain


MESH = pl.DeviceIdType.MESH
BF16 = jnp.bfloat16
F32 = jnp.float32


def layer_kernel(
    n,
    experts,
    lengths,
    lambdas,
    tokens,
    trig,
    gain_first,
    head_gain,
    gain_second,
    routes,
    w_small,
    wq_hbm,
    wk_hbm,
    wv_hbm,
    keys_hbm,
    values_hbm,
    wo_hbm,
    wg_hbm,
    wu_hbm,
    wd_hbm,
    dg_hbm,
    du_hbm,
    dd_hbm,
    out,
    wqkv,
    keys,
    values,
    wo,
    q8,
    scores,
    mixed,
    heads,
    resid,
    buf,
    wgu,
    dgu,
    wd,
    dd,
    ehid,
    dhid,
    stage,
    mine,
    rbuf,
    local_sem,
    xs,
    xr,
    gs,
    gr,
    fs,
    fr,
    ws,
    wr,
    hs,
    hr,
    rs,
    rr,
):
    me = lax.axis_index("ep")
    core = lax.axis_index("tp")
    other = 1 - core
    seqs, width = tokens.shape
    half = width // 2
    ffe = wg_hbm.shape[2]
    ffd = dg_hbm.shape[1]
    group = head_gain.shape[0]
    span = keys.shape[1]
    partner = (me, other)

    local = []

    def fetch(src, dst):
        copy = pltpu.make_async_copy(src, dst, local_sem.at[len(local)])
        copy.start()
        local.append(copy)

    qw, kw, vw = wq_hbm.shape[1], wk_hbm.shape[1], wv_hbm.shape[1]
    fetch(wq_hbm, wqkv.at[:, pl.ds(0, qw)])
    fetch(wk_hbm, wqkv.at[:, pl.ds(qw, kw)])
    fetch(wv_hbm, wqkv.at[:, pl.ds(qw + kw, vw)])
    parts = 4
    step = seqs // parts
    for p in range(parts):
        fetch(keys_hbm.at[pl.ds(p * step, step)], keys.at[pl.ds(p * step, step)])

    barrier = pltpu.get_barrier_semaphore()

    def greet(d, carry):
        pl.semaphore_signal(
            barrier, inc=1, device_id=(lax.rem(me + d, n), core), device_id_type=MESH
        )
        return carry

    pl.semaphore_signal(barrier, inc=1, device_id=partner, device_id_type=MESH)
    lax.fori_loop(1, n, greet, 0)

    floats = tokens[...].astype(F32)
    normed = norm(floats, gain_first[...]).astype(BF16)
    for copy in local[:3]:
        copy.wait()
    for p in range(parts):
        fetch(values_hbm.at[pl.ds(p * step, step)], values.at[pl.ds(p * step, step)])
    fetch(wo_hbm, wo)
    fetch(dg_hbm, dgu.at[:, pl.ds(0, ffd)])
    fetch(du_hbm, dgu.at[:, pl.ds(ffd, ffd)])
    fetch(wg_hbm.at[0], wgu.at[:, pl.ds(0, ffe)])
    fetch(wu_hbm.at[0], wgu.at[:, pl.ds(ffe, ffe)])
    mine_cols = pl.ds(pl.multiple_of(core * half, 128), half)
    fetch(wd_hbm.at[0, :, mine_cols], wd.at[0])
    fetch(dd_hbm.at[:, mine_cols], dd.at[0])
    proj = jnp.dot(normed, wqkv[...], preferred_element_type=F32)
    cosine, sine = trig[0], trig[1]
    lane = lax.broadcasted_iota(jnp.int32, cosine.shape, 1)
    upper = lane % HD >= HD // 2

    def rotated(x):
        swapped = jnp.where(upper, pltpu.roll(x, HD // 2, 1), pltpu.roll(x, 2 * HD - HD // 2, 1))
        return (x * cosine + swapped * sine).astype(BF16).astype(F32)

    for g in range(group):
        query = rotated(proj[:, g * 2 * HD : (g + 1) * 2 * HD])
        for c in range(2):
            q8[:, c * group + g, :] = jnp.where(lane // HD == c, query, 0.0)
    key_new = rotated(proj[:, qw : qw + kw])
    value_new = proj[:, qw + kw :].astype(BF16).astype(F32)

    pl.semaphore_wait(barrier, n)
    their_cols = pl.ds(pl.multiple_of(other * half, 128), half)
    give_wd = pltpu.make_async_remote_copy(
        src_ref=wd_hbm.at[0, :, their_cols],
        dst_ref=wd.at[1],
        send_sem=ws.at[0],
        recv_sem=wr.at[0],
        device_id=partner,
        device_id_type=MESH,
    )
    give_wd.start()
    give_dd = pltpu.make_async_remote_copy(
        src_ref=dd_hbm.at[:, their_cols],
        dst_ref=dd.at[1],
        send_sem=ws.at[1],
        recv_sem=wr.at[1],
        device_id=partner,
        device_id_type=MESH,
    )
    give_dd.start()

    scale = HD ** (-0.5)
    place = lax.broadcasted_iota(jnp.int32, (2 * group, span), 1)
    for p in range(parts):
        local[3 + p].wait()
        for s in range(p * step, (p + 1) * step):
            score = lax.dot_general(
                q8[s].astype(BF16),
                keys[s],
                (((1,), (1,)), ((), ())),
                preferred_element_type=F32,
            )
            scores[s] = jnp.where(place < lengths[s], score * scale, -jnp.inf)
    row = lax.broadcasted_iota(jnp.int32, (2 * group, 1), 0)
    lam = jnp.zeros((2 * group, 1), F32)
    for g in range(group):
        lam = jnp.where(row == g, lambdas[g], lam)
    gain = jnp.concatenate([head_gain[...], head_gain[...]], 0)
    for p in range(parts):
        at = slice(p * step, (p + 1) * step)
        own = jnp.sum(q8[at] * key_new[at][:, None, :], -1, keepdims=True) * scale
        score = scores[at]
        top = jnp.maximum(jnp.max(score, -1, keepdims=True), own)
        expo = jnp.exp(score - top)
        own_e = jnp.exp(own - top)
        total = 1.0 / (jnp.sum(expo, -1, keepdims=True) + own_e)
        probs = expo * total
        own_p = own_e * total
        flipped = jnp.concatenate([probs[:, group:], probs[:, :group]], 1)
        own_flipped = jnp.concatenate([own_p[:, group:], own_p[:, :group]], 1)
        weights = (probs - lam[None] * flipped).astype(BF16)
        own_w = (own_p - lam[None] * own_flipped).astype(BF16).astype(F32)
        local[3 + parts + p].wait()
        for s in range(step):
            mixed[p * step + s] = jnp.dot(
                weights[s], values[p * step + s], preferred_element_type=F32
            )
        mix = mixed[at] + own_w * value_new[at][:, None, :]
        square = jnp.mean(mix * mix, -1, keepdims=True)
        mixed[at] = mix * lax.rsqrt(square + 1e-05) * gain[None]
    for g in range(group):
        heads[core, :, g * VD : (g + 1) * VD] = mixed[:, g, :].astype(BF16)
    swap = pltpu.make_async_remote_copy(
        src_ref=heads.at[core],
        dst_ref=heads.at[core],
        send_sem=xs.at[0],
        recv_sem=xr.at[0],
        device_id=partner,
        device_id_type=MESH,
    )
    swap.start()
    local[3 + 2 * parts].wait()
    deep = group * VD
    after = floats + jnp.dot(
        heads[core],
        wo[pl.ds(pl.multiple_of(core * deep, deep), deep)],
        preferred_element_type=F32,
    )
    swap.wait_recv()
    after += jnp.dot(
        heads[other],
        wo[pl.ds(pl.multiple_of(other * deep, deep), deep)],
        preferred_element_type=F32,
    )
    resid[...] = after
    moe_in = norm(after, gain_second[...]).astype(BF16)
    logits = jnp.dot(moe_in, w_small[...], preferred_element_type=F32)
    spot = lax.broadcasted_iota(jnp.int32, logits.shape, 1)
    hit = spot == routes[:, 0:1]
    for k in range(1, routes.shape[1]):
        hit = hit | (spot == routes[:, k : k + 1])
    chosen = jnp.where(hit, logits, -jnp.inf)
    chosen = jnp.exp(chosen - jnp.max(chosen, -1, keepdims=True))
    chosen = chosen / jnp.sum(chosen, -1, keepdims=True)
    grouped = (spot >= experts) & (spot < experts + N_GROUPS)
    groups = jnp.where(grouped, logits, -jnp.inf)
    groups = jnp.exp(groups - jnp.max(groups, -1, keepdims=True))
    groups = groups / jnp.sum(groups, -1, keepdims=True)
    per_group = experts // N_GROUPS
    part = jnp.zeros(logits.shape, F32)
    for g in range(N_GROUPS):
        one = jnp.sum(jnp.where(spot == experts + g, groups, 0.0), -1, keepdims=True)
        part = jnp.where(spot // per_group == g, one, part)
    blend_here = jnp.where(spot == experts + N_GROUPS, jax.nn.sigmoid(logits), 0.0)
    extra_here = jnp.where(hit, part * chosen, blend_here).astype(BF16)
    for h in range(2):
        buf[me, h, :, :half] = moe_in[:, h * half : (h + 1) * half]
        buf[me, h, :, half:] = extra_here

    def gather_copy(d):
        return pltpu.make_async_remote_copy(
            src_ref=buf.at[me, core],
            dst_ref=buf.at[me, core],
            send_sem=gs.at[d],
            recv_sem=gr.at[d],
            device_id=(lax.rem(me + d, n), core),
            device_id_type=MESH,
        )

    def gather_start(d, carry):
        gather_copy(d).start()
        return carry

    lax.fori_loop(1, n, gather_start, 0)

    def forward_copy(d):
        source = lax.rem(me - d + n, n)
        return pltpu.make_async_remote_copy(
            src_ref=buf.at[source, core],
            dst_ref=buf.at[source, core],
            send_sem=fs.at[d],
            recv_sem=fr.at[d],
            device_id=partner,
            device_id_type=MESH,
        )

    def forward(d, carry):
        gather_copy(d).wait_recv()
        forward_copy(d).start()
        return carry

    lax.fori_loop(1, n, forward, 0)

    def forward_done(d, carry):
        forward_copy(d).wait_recv()
        return carry

    lax.fori_loop(1, n, forward_done, 0)
    for copy in local[4 + 2 * parts :]:
        copy.wait()

    blocks = min(n, max(1, 256 // seqs))
    rows = blocks * seqs

    def weights_of(j):
        extra = buf[pl.ds(j * blocks, blocks), 0, :, half:].reshape(rows, -1).astype(F32)
        lane = lax.broadcasted_iota(jnp.int32, extra.shape, 1)
        column = jnp.sum(jnp.where(lane == me, extra, 0.0), -1, keepdims=True)
        blend = jnp.sum(jnp.where(lane == experts + N_GROUPS, extra, 0.0), -1, keepdims=True)
        return column, blend

    def up(j, carry):
        _, blend = weights_of(j)
        at = pl.ds(pl.multiple_of(j * rows, rows), rows)
        dense = jnp.zeros((rows, 2 * ffd), F32)
        expert = jnp.zeros((rows, 2 * ffe), F32)
        for h in range(width // half):
            x = buf[pl.ds(j * blocks, blocks), h, :, :half].reshape(rows, half)
            dense += jnp.dot(x, dgu[h * half : (h + 1) * half], preferred_element_type=F32)
            expert += jnp.dot(x, wgu[h * half : (h + 1) * half], preferred_element_type=F32)
        dhid[0, at] = (blend * jax.nn.silu(dense[:, :ffd]) * dense[:, ffd:]).astype(BF16)
        ehid[0, at] = (jax.nn.silu(expert[:, :ffe]) * expert[:, ffe:]).astype(BF16)
        return carry

    lax.fori_loop(0, n // blocks, up, 0)

    give = []
    for k, hid in enumerate((dhid, ehid)):
        copy = pltpu.make_async_remote_copy(
            src_ref=hid.at[0],
            dst_ref=hid.at[1],
            send_sem=hs.at[k],
            recv_sem=hr.at[k],
            device_id=partner,
            device_id_type=MESH,
        )
        copy.start()
        give.append(copy)
    give_wd.wait_recv()
    give_dd.wait_recv()
    for copy in give:
        copy.wait_recv()

    def down(j, carry):
        column, _ = weights_of(j)
        at = pl.ds(pl.multiple_of(j * rows, rows), rows)
        expert = jnp.dot(ehid[0, at], wd[0], preferred_element_type=F32)
        expert += jnp.dot(ehid[1, at], wd[1], preferred_element_type=F32)
        dense = jnp.dot(dhid[0, at], dd[0], preferred_element_type=F32)
        dense += jnp.dot(dhid[1, at], dd[1], preferred_element_type=F32)
        term = dense + column * expert
        stage[pl.ds(j * blocks, blocks)] = term.reshape(blocks, seqs, half).astype(BF16)
        return carry

    lax.fori_loop(0, n // blocks, down, 0)

    def scatter_copy(d):
        target = lax.rem(me + d, n)
        return pltpu.make_async_remote_copy(
            src_ref=stage.at[target],
            dst_ref=rbuf.at[d],
            send_sem=rs.at[d],
            recv_sem=rr.at[d],
            device_id=(target, core),
            device_id_type=MESH,
        )

    def scatter_start(d, carry):
        scatter_copy(d).start()
        return carry

    lax.fori_loop(1, n, scatter_start, 0)
    mine[...] = resid[:, mine_cols] + stage[me].astype(F32)

    def collect(d, carry):
        scatter_copy(d).wait_recv()
        mine[...] += rbuf[d].astype(F32)
        return carry

    lax.fori_loop(1, n, collect, 0)
    out[...] = mine[...].astype(BF16)

    def drain(d, carry):
        gather_copy(d).wait_send()
        forward_copy(d).wait_send()
        scatter_copy(d).wait_send()
        return carry

    lax.fori_loop(1, n, drain, 0)
    swap.wait_send()
    give_wd.wait_send()
    give_dd.wait_send()
    for copy in give:
        copy.wait_send()


def local(
    tokens,
    lengths,
    gain_first,
    w_query,
    w_key,
    w_value,
    cache_keys,
    cache_values,
    lambdas,
    head_gain,
    w_output,
    gain_second,
    w_group,
    w_router,
    w_blend,
    routes,
    w_eg,
    w_eu,
    w_ed,
    w_dg,
    w_du,
    w_dd,
):
    n = lax.axis_size("ep")
    seqs, width = tokens.shape
    half = width // lax.axis_size("tp")
    span = cache_keys.shape[1]
    experts = w_router.shape[1]
    group = lambdas.shape[0]
    inverse = 10000.0 ** (-jnp.arange(HD // 2, dtype=F32) / (HD // 2))
    angle = lengths.astype(F32)[:, None] * inverse
    cosine, sine = jnp.cos(angle), jnp.sin(angle)
    trig = jnp.stack(
        [jnp.concatenate([cosine] * 4, 1), jnp.concatenate([-sine, sine, -sine, sine], 1)]
    )
    w_small = jnp.concatenate([w_router, w_group, w_blend[:, None]], 1)
    w_small = jnp.pad(w_small, ((0, 0), (0, -w_small.shape[1] % 128)))
    lanes = w_small.shape[1]
    spare = -w_dg.shape[1] % 128
    if spare:
        w_dg = jnp.pad(w_dg, ((0, 0), (0, spare)))
        w_du = jnp.pad(w_du, ((0, 0), (0, spare)))
        w_dd = jnp.pad(w_dd, ((0, spare), (0, 0)))
    ffe, ffd = w_eg.shape[2], w_dg.shape[1]
    dma = pltpu.SemaphoreType.DMA
    smem = pl.BlockSpec(memory_space=pltpu.SMEM)
    vmem = pl.BlockSpec(memory_space=pltpu.VMEM)
    anywhere = pl.BlockSpec(memory_space=pl.ANY)
    total = n * seqs
    columns = w_query.shape[1] + w_key.shape[1] + w_value.shape[1]
    return pl.pallas_call(
        functools.partial(layer_kernel, n, experts),
        out_shape=jax.ShapeDtypeStruct((seqs, half), BF16),
        in_specs=[smem] * 2 + [vmem] * 7 + [anywhere] * 12,
        out_specs=vmem,
        scratch_shapes=[
            pltpu.VMEM((width, columns), BF16),
            pltpu.VMEM(cache_keys.shape, BF16),
            pltpu.VMEM(cache_values.shape, BF16),
            pltpu.VMEM(w_output.shape, BF16),
            pltpu.VMEM((seqs, 2 * group, 2 * HD), F32),
            pltpu.VMEM((seqs, 2 * group, span), F32),
            pltpu.VMEM((seqs, 2 * group, VD), F32),
            pltpu.VMEM((2, seqs, group * VD), BF16),
            pltpu.VMEM((seqs, width), F32),
            pltpu.VMEM((n, 2, seqs, half + lanes), BF16),
            pltpu.VMEM((width, 2 * ffe), BF16),
            pltpu.VMEM((width, 2 * ffd), BF16),
            pltpu.VMEM((2, ffe, half), BF16),
            pltpu.VMEM((2, ffd, half), BF16),
            pltpu.VMEM((2, total, ffe), BF16),
            pltpu.VMEM((2, total, ffd), BF16),
            pltpu.VMEM((n, seqs, half), BF16),
            pltpu.VMEM((seqs, half), F32),
            pltpu.VMEM((n, seqs, half), BF16),
            dma((18,)),
            dma((1,)),
            dma((1,)),
            dma((n,)),
            dma((n,)),
            dma((n,)),
            dma((n,)),
            dma((2,)),
            dma((2,)),
            dma((2,)),
            dma((2,)),
            dma((n,)),
            dma((n,)),
        ],
        compiler_params=pltpu.CompilerParams(collective_id=0, has_side_effects=True),
        name="layer",
    )(
        lengths,
        lambdas,
        tokens,
        trig,
        gain_first.reshape(1, -1),
        head_gain,
        gain_second.reshape(1, -1),
        routes,
        w_small,
        w_query,
        w_key,
        w_value,
        cache_keys,
        cache_values,
        w_output,
        w_eg,
        w_eu,
        w_ed,
        w_dg,
        w_du,
        w_dd,
    )


def solution(mesh):
    return jax.shard_map(
        local,
        mesh=mesh,
        in_specs=(
            P("ep", None),
            P("ep"),
            P(),
            P(None, "tp"),
            P(None, "tp"),
            P(None, "tp"),
            P("ep", None, "tp"),
            P("ep", None, "tp"),
            P("tp"),
            P("tp", None),
            P(),
            P(),
            P(),
            P(),
            P(),
            P("ep", None),
            P("ep", None, "tp"),
            P("ep", None, "tp"),
            P("ep", "tp", None),
            P(None, ("ep", "tp")),
            P(None, ("ep", "tp")),
            P(("ep", "tp"), None),
        ),
        out_specs=P("ep", "tp"),
        check_vma=False,
    )
```

```python
import functools

import jax
import jax.numpy as jnp
import numpy as np
from jax import lax
from jax.experimental import pallas as pl
from jax.experimental.pallas import tpu as pltpu
from jax.sharding import PartitionSpec as P

HD = 64
VD = 128
N_GROUPS = 4


def norm(floats, gain):
    center = floats - jnp.mean(floats, -1, keepdims=True)
    spread = jnp.mean(center * center, -1, keepdims=True)
    return center * lax.rsqrt(spread + 1e-05) * gain


MESH = pl.DeviceIdType.MESH
BF16 = jnp.bfloat16
F32 = jnp.float32


def layer_kernel(
    n,
    experts,
    lengths,
    lambdas,
    tokens,
    inverse,
    gain_first,
    head_gain,
    gain_second,
    routes,
    w_small,
    wq_hbm,
    wk_hbm,
    wv_hbm,
    keys_hbm,
    values_hbm,
    wo_hbm,
    wg_hbm,
    wu_hbm,
    wd_hbm,
    dg_hbm,
    du_hbm,
    dd_hbm,
    out,
    wqkv,
    keys,
    values,
    wo,
    q8,
    scores,
    mixed,
    heads,
    resid,
    buf,
    wgu,
    dgu,
    wd,
    dd,
    ehid,
    dhid,
    stage,
    mine,
    near,
    sums,
    far,
    local_sem,
    xs,
    xr,
    gz,
    gs,
    gr,
    fs,
    fr,
    ws,
    wr,
    hs,
    hr,
    rs,
    rr,
    zs,
    zr,
):
    me = lax.axis_index("ep")
    core = lax.axis_index("tp")
    other = 1 - core
    seqs, width = tokens.shape
    half = width // 2
    ffe = wg_hbm.shape[2]
    ffd = dg_hbm.shape[1]
    group = head_gain.shape[0]
    span = keys.shape[1]
    partner = (me, other)

    local = []

    def fetch(src, dst):
        copy = pltpu.make_async_copy(src, dst, local_sem.at[len(local)])
        copy.start()
        local.append(copy)

    qw, kw, vw = wq_hbm.shape[1], wk_hbm.shape[1], wv_hbm.shape[1]
    fetch(wq_hbm, wqkv.at[:, pl.ds(0, qw)])
    fetch(wk_hbm, wqkv.at[:, pl.ds(qw, kw)])
    fetch(wv_hbm, wqkv.at[:, pl.ds(qw + kw, vw)])
    parts = 4
    step = seqs // parts
    for p in range(parts):
        fetch(keys_hbm.at[pl.ds(p * step, step)], keys.at[pl.ds(p * step, step)])

    barrier = pltpu.get_barrier_semaphore()

    depth = 4 if n % 4 == 0 else 1
    plane = n // depth
    level, spot_here = me // plane, lax.rem(me, plane)

    def level_mate(d):
        return lax.rem(level + d, depth) * plane + spot_here

    def plane_mate(d):
        return level * plane + lax.rem(spot_here + d, plane)

    def greet(target):
        pl.semaphore_signal(barrier, inc=1, device_id=target, device_id_type=MESH)

    def greet_plane(d, carry):
        greet((plane_mate(d), core))
        return carry

    greet(partner)
    for d in range(1, depth):
        greet((level_mate(d), core))
    lax.fori_loop(1, plane, greet_plane, 0)

    lane = lax.broadcasted_iota(jnp.int32, (seqs, 2 * HD), 1)
    line = lax.broadcasted_iota(jnp.int32, (seqs, 2 * HD), 0)
    upper = lane % HD >= HD // 2
    position = jnp.zeros((seqs, 2 * HD), jnp.int32)
    for s in range(seqs):
        position = jnp.where(line == s, lengths[s], position)
    angle = position.astype(F32) * inverse[...]
    cosine = jnp.cos(angle)
    sine = jnp.where(upper, jnp.sin(angle), -jnp.sin(angle))
    floats = tokens[...].astype(F32)
    normed = norm(floats, gain_first[...]).astype(BF16)
    for copy in local[:3]:
        copy.wait()
    for p in range(parts):
        fetch(values_hbm.at[pl.ds(p * step, step)], values.at[pl.ds(p * step, step)])
    fetch(wo_hbm, wo)
    fetch(dg_hbm, dgu.at[:, pl.ds(0, ffd)])
    fetch(du_hbm, dgu.at[:, pl.ds(ffd, ffd)])
    fetch(wg_hbm.at[0], wgu.at[:, pl.ds(0, ffe)])
    fetch(wu_hbm.at[0], wgu.at[:, pl.ds(ffe, ffe)])
    mine_cols = pl.ds(pl.multiple_of(core * half, 128), half)
    fetch(wd_hbm.at[0, :, mine_cols], wd.at[0])
    fetch(dd_hbm.at[:, mine_cols], dd.at[0])
    proj = jnp.dot(normed, wqkv[...], preferred_element_type=F32)

    def rotated(x):
        swapped = jnp.where(upper, pltpu.roll(x, HD // 2, 1), pltpu.roll(x, 2 * HD - HD // 2, 1))
        return (x * cosine + swapped * sine).astype(BF16).astype(F32)

    for g in range(group):
        query = rotated(proj[:, g * 2 * HD : (g + 1) * 2 * HD])
        for c in range(2):
            q8[:, c * group + g, :] = jnp.where(lane // HD == c, query, 0.0)
    key_new = rotated(proj[:, qw : qw + kw])
    value_new = proj[:, qw + kw :].astype(BF16).astype(F32)

    pl.semaphore_wait(barrier, depth + plane - 1)
    their_cols = pl.ds(pl.multiple_of(other * half, 128), half)
    give_wd = pltpu.make_async_remote_copy(
        src_ref=wd_hbm.at[0, :, their_cols],
        dst_ref=wd.at[1],
        send_sem=ws.at[0],
        recv_sem=wr.at[0],
        device_id=partner,
        device_id_type=MESH,
    )
    give_wd.start()
    give_dd = pltpu.make_async_remote_copy(
        src_ref=dd_hbm.at[:, their_cols],
        dst_ref=dd.at[1],
        send_sem=ws.at[1],
        recv_sem=wr.at[1],
        device_id=partner,
        device_id_type=MESH,
    )
    give_dd.start()

    scale = HD ** (-0.5)
    place = lax.broadcasted_iota(jnp.int32, (2 * group, span), 1)
    for p in range(parts):
        local[3 + p].wait()
        for s in range(p * step, (p + 1) * step):
            score = lax.dot_general(
                q8[s].astype(BF16),
                keys[s],
                (((1,), (1,)), ((), ())),
                preferred_element_type=F32,
            )
            scores[s] = jnp.where(place < lengths[s], score * scale, -jnp.inf)
    row = lax.broadcasted_iota(jnp.int32, (2 * group, 1), 0)
    lam = jnp.zeros((2 * group, 1), F32)
    for g in range(group):
        lam = jnp.where(row == g, lambdas[g], lam)
    gain = jnp.concatenate([head_gain[...], head_gain[...]], 0)
    for p in range(parts):
        at = slice(p * step, (p + 1) * step)
        own = jnp.sum(q8[at] * key_new[at][:, None, :], -1, keepdims=True) * scale
        score = scores[at]
        top = jnp.maximum(jnp.max(score, -1, keepdims=True), own)
        expo = jnp.exp(score - top)
        own_e = jnp.exp(own - top)
        total = 1.0 / (jnp.sum(expo, -1, keepdims=True) + own_e)
        probs = expo * total
        own_p = own_e * total
        flipped = jnp.concatenate([probs[:, group:], probs[:, :group]], 1)
        own_flipped = jnp.concatenate([own_p[:, group:], own_p[:, :group]], 1)
        weights = (probs - lam[None] * flipped).astype(BF16)
        own_w = (own_p - lam[None] * own_flipped).astype(BF16).astype(F32)
        local[3 + parts + p].wait()
        for s in range(step):
            mixed[p * step + s] = jnp.dot(
                weights[s], values[p * step + s], preferred_element_type=F32
            )
        mix = mixed[at] + own_w * value_new[at][:, None, :]
        square = jnp.mean(mix * mix, -1, keepdims=True)
        mixed[at] = mix * lax.rsqrt(square + 1e-05) * gain[None]
    for g in range(group):
        heads[core, :, g * VD : (g + 1) * VD] = mixed[:, g, :].astype(BF16)
    swap = pltpu.make_async_remote_copy(
        src_ref=heads.at[core],
        dst_ref=heads.at[core],
        send_sem=xs.at[0],
        recv_sem=xr.at[0],
        device_id=partner,
        device_id_type=MESH,
    )
    swap.start()
    local[3 + 2 * parts].wait()
    deep = group * VD
    after = floats + jnp.dot(
        heads[core],
        wo[pl.ds(pl.multiple_of(core * deep, deep), deep)],
        preferred_element_type=F32,
    )
    swap.wait_recv()
    after += jnp.dot(
        heads[other],
        wo[pl.ds(pl.multiple_of(other * deep, deep), deep)],
        preferred_element_type=F32,
    )
    resid[...] = after
    moe_in = norm(after, gain_second[...]).astype(BF16)
    logits = jnp.dot(moe_in, w_small[...], preferred_element_type=F32)
    spot = lax.broadcasted_iota(jnp.int32, logits.shape, 1)
    hit = spot == routes[:, 0:1]
    for k in range(1, routes.shape[1]):
        hit = hit | (spot == routes[:, k : k + 1])
    chosen = jnp.where(hit, logits, -jnp.inf)
    chosen = jnp.exp(chosen - jnp.max(chosen, -1, keepdims=True))
    chosen = chosen / jnp.sum(chosen, -1, keepdims=True)
    grouped = (spot >= experts) & (spot < experts + N_GROUPS)
    groups = jnp.where(grouped, logits, -jnp.inf)
    groups = jnp.exp(groups - jnp.max(groups, -1, keepdims=True))
    groups = groups / jnp.sum(groups, -1, keepdims=True)
    per_group = experts // N_GROUPS
    part = jnp.zeros(logits.shape, F32)
    for g in range(N_GROUPS):
        one = jnp.sum(jnp.where(spot == experts + g, groups, 0.0), -1, keepdims=True)
        part = jnp.where(spot // per_group == g, one, part)
    blend_here = jnp.where(spot == experts + N_GROUPS, jax.nn.sigmoid(logits), 0.0)
    extra_here = jnp.where(hit, part * chosen, blend_here).astype(BF16)
    for h in range(2):
        buf[me, h, :, :half] = moe_in[:, h * half : (h + 1) * half]
        buf[me, h, :, half:] = extra_here

    def gather_copy(source, target, send_sem):
        return pltpu.make_async_remote_copy(
            src_ref=buf.at[source, core],
            dst_ref=buf.at[source, core],
            send_sem=send_sem,
            recv_sem=gr.at[source],
            device_id=(target, core),
            device_id_type=MESH,
        )

    def level_copy(d):
        return gather_copy(me, level_mate(d), gz.at[d])

    def plane_copy(d, k):
        return gather_copy(level_mate(d), plane_mate(k), gs.at[d * plane + k])

    def forward_copy(source):
        return pltpu.make_async_remote_copy(
            src_ref=buf.at[source, core],
            dst_ref=buf.at[source, core],
            send_sem=fs.at[source],
            recv_sem=fr.at[source],
            device_id=partner,
            device_id_type=MESH,
        )

    def share(d):
        def start(k, carry):
            plane_copy(d, k).start()
            return carry

        lax.fori_loop(1, plane, start, 0)

    def arrive(source):
        gather_copy(source, source, gz.at[0]).wait_recv()

    for d in range(1, depth):
        level_copy(d).start()
    share(0)
    for d in range(1, depth):
        arrive(level_mate(d))
        share(d)
        forward_copy(level_mate(d)).start()
    for d in range(depth):

        def forward(k, carry, d=d):
            source = lax.rem(level + d, depth) * plane + lax.rem(spot_here + k, plane)
            arrive(source)
            forward_copy(source).start()
            return carry

        lax.fori_loop(1, plane, forward, 0)

    def forward_done(d, carry):
        forward_copy(lax.rem(me + d, n)).wait_recv()
        return carry

    lax.fori_loop(1, n, forward_done, 0)
    for copy in local[4 + 2 * parts :]:
        copy.wait()

    blocks = min(n, max(1, 256 // seqs))
    rows = blocks * seqs

    def weights_of(j):
        extra = buf[pl.ds(j * blocks, blocks), 0, :, half:].reshape(rows, -1).astype(F32)
        lane = lax.broadcasted_iota(jnp.int32, extra.shape, 1)
        column = jnp.sum(jnp.where(lane == me, extra, 0.0), -1, keepdims=True)
        blend = jnp.sum(jnp.where(lane == experts + N_GROUPS, extra, 0.0), -1, keepdims=True)
        return column, blend

    def up(j, carry):
        _, blend = weights_of(j)
        at = pl.ds(pl.multiple_of(j * rows, rows), rows)
        dense = jnp.zeros((rows, 2 * ffd), F32)
        expert = jnp.zeros((rows, 2 * ffe), F32)
        for h in range(width // half):
            x = buf[pl.ds(j * blocks, blocks), h, :, :half].reshape(rows, half)
            dense += jnp.dot(x, dgu[h * half : (h + 1) * half], preferred_element_type=F32)
            expert += jnp.dot(x, wgu[h * half : (h + 1) * half], preferred_element_type=F32)
        dhid[0, at] = (blend * jax.nn.silu(dense[:, :ffd]) * dense[:, ffd:]).astype(BF16)
        ehid[0, at] = (jax.nn.silu(expert[:, :ffe]) * expert[:, ffe:]).astype(BF16)
        return carry

    lax.fori_loop(0, n // blocks, up, 0)

    give = []
    for k, hid in enumerate((dhid, ehid)):
        copy = pltpu.make_async_remote_copy(
            src_ref=hid.at[0],
            dst_ref=hid.at[1],
            send_sem=hs.at[k],
            recv_sem=hr.at[k],
            device_id=partner,
            device_id_type=MESH,
        )
        copy.start()
        give.append(copy)
    give_wd.wait_recv()
    give_dd.wait_recv()
    for copy in give:
        copy.wait_recv()

    def down(j, carry):
        column, _ = weights_of(j)
        at = pl.ds(pl.multiple_of(j * rows, rows), rows)
        expert = jnp.dot(ehid[0, at], wd[0], preferred_element_type=F32)
        expert += jnp.dot(ehid[1, at], wd[1], preferred_element_type=F32)
        dense = jnp.dot(dhid[0, at], dd[0], preferred_element_type=F32)
        dense += jnp.dot(dhid[1, at], dd[1], preferred_element_type=F32)
        term = dense + column * expert
        stage[pl.ds(j * blocks, blocks)] = term.reshape(blocks, seqs, half).astype(BF16)
        return carry

    lax.fori_loop(0, n // blocks, down, 0)

    def near_copy(d, k):
        return pltpu.make_async_remote_copy(
            src_ref=stage.at[lax.rem(level + d, depth) * plane + lax.rem(spot_here + k, plane)],
            dst_ref=near.at[d * plane + k],
            send_sem=rs.at[d * plane + k],
            recv_sem=rr.at[d * plane + k],
            device_id=(plane_mate(k), core),
            device_id_type=MESH,
        )

    def far_copy(d):
        return pltpu.make_async_remote_copy(
            src_ref=sums.at[d],
            dst_ref=far.at[d],
            send_sem=zs.at[d],
            recv_sem=zr.at[d],
            device_id=(level_mate(d), core),
            device_id_type=MESH,
        )

    order = list(range(1, depth)) + [0]
    for d in order:

        def near_start(k, carry, d=d):
            near_copy(d, k).start()
            return carry

        lax.fori_loop(1, plane, near_start, 0)
    for d in order:
        if d:
            mine[...] = stage[level_mate(d)].astype(F32)
        else:
            mine[...] = resid[:, mine_cols] + stage[me].astype(F32)

        def near_add(k, carry, d=d):
            near_copy(d, k).wait_recv()
            mine[...] += near[d * plane + k].astype(F32)
            return carry

        lax.fori_loop(1, plane, near_add, 0)
        if d:
            sums[d] = mine[...].astype(BF16)
            far_copy(d).start()
    for d in range(1, depth):
        far_copy(d).wait_recv()
        mine[...] += far[d].astype(F32)
    out[...] = mine[...].astype(BF16)

    for d in range(depth):

        def drain(k, carry, d=d):
            plane_copy(d, k).wait_send()
            near_copy(d, k).wait_send()
            return carry

        lax.fori_loop(1, plane, drain, 0)
        if d:
            level_copy(d).wait_send()
            far_copy(d).wait_send()

    def forward_drain(d, carry):
        forward_copy(lax.rem(me + d, n)).wait_send()
        return carry

    lax.fori_loop(1, n, forward_drain, 0)
    swap.wait_send()
    give_wd.wait_send()
    give_dd.wait_send()
    for copy in give:
        copy.wait_send()


def local(
    tokens,
    lengths,
    gain_first,
    w_query,
    w_key,
    w_value,
    cache_keys,
    cache_values,
    lambdas,
    head_gain,
    w_output,
    gain_second,
    w_group,
    w_router,
    w_blend,
    routes,
    w_eg,
    w_eu,
    w_ed,
    w_dg,
    w_du,
    w_dd,
):
    n = lax.axis_size("ep")
    seqs, width = tokens.shape
    half = width // lax.axis_size("tp")
    span = cache_keys.shape[1]
    experts = w_router.shape[1]
    group = lambdas.shape[0]
    inverse = 10000.0 ** (-np.arange(HD // 2, dtype=np.float32) / np.float32(HD // 2))
    inverse = jnp.asarray(np.tile(inverse.astype(np.float32), 4)[None])
    w_small = jnp.concatenate([w_router, w_group, w_blend[:, None]], 1)
    w_small = jnp.pad(w_small, ((0, 0), (0, -w_small.shape[1] % 128)))
    lanes = w_small.shape[1]
    spare = -w_dg.shape[1] % 128
    if spare:
        w_dg = jnp.pad(w_dg, ((0, 0), (0, spare)))
        w_du = jnp.pad(w_du, ((0, 0), (0, spare)))
        w_dd = jnp.pad(w_dd, ((0, spare), (0, 0)))
    ffe, ffd = w_eg.shape[2], w_dg.shape[1]
    dma = pltpu.SemaphoreType.DMA
    smem = pl.BlockSpec(memory_space=pltpu.SMEM)
    vmem = pl.BlockSpec(memory_space=pltpu.VMEM)
    anywhere = pl.BlockSpec(memory_space=pl.ANY)
    total = n * seqs
    columns = w_query.shape[1] + w_key.shape[1] + w_value.shape[1]
    return pl.pallas_call(
        functools.partial(layer_kernel, n, experts),
        out_shape=jax.ShapeDtypeStruct((seqs, half), BF16),
        in_specs=[smem] * 2 + [vmem] * 7 + [anywhere] * 12,
        out_specs=vmem,
        scratch_shapes=[
            pltpu.VMEM((width, columns), BF16),
            pltpu.VMEM(cache_keys.shape, BF16),
            pltpu.VMEM(cache_values.shape, BF16),
            pltpu.VMEM(w_output.shape, BF16),
            pltpu.VMEM((seqs, 2 * group, 2 * HD), F32),
            pltpu.VMEM((seqs, 2 * group, span), F32),
            pltpu.VMEM((seqs, 2 * group, VD), F32),
            pltpu.VMEM((2, seqs, group * VD), BF16),
            pltpu.VMEM((seqs, width), F32),
            pltpu.VMEM((n, 2, seqs, half + lanes), BF16),
            pltpu.VMEM((width, 2 * ffe), BF16),
            pltpu.VMEM((width, 2 * ffd), BF16),
            pltpu.VMEM((2, ffe, half), BF16),
            pltpu.VMEM((2, ffd, half), BF16),
            pltpu.VMEM((2, total, ffe), BF16),
            pltpu.VMEM((2, total, ffd), BF16),
            pltpu.VMEM((n, seqs, half), BF16),
            pltpu.VMEM((seqs, half), F32),
            pltpu.VMEM((n, seqs, half), BF16),
            pltpu.VMEM((4, seqs, half), BF16),
            pltpu.VMEM((4, seqs, half), BF16),
            dma((18,)),
            dma((1,)),
            dma((1,)),
            dma((4,)),
            dma((n,)),
            dma((n,)),
            dma((n,)),
            dma((n,)),
            dma((2,)),
            dma((2,)),
            dma((2,)),
            dma((2,)),
            dma((n,)),
            dma((n,)),
            dma((4,)),
            dma((4,)),
        ],
        compiler_params=pltpu.CompilerParams(collective_id=0, has_side_effects=True),
        name="layer",
    )(
        lengths,
        lambdas,
        tokens,
        inverse,
        gain_first.reshape(1, -1),
        head_gain,
        gain_second.reshape(1, -1),
        routes,
        w_small,
        w_query,
        w_key,
        w_value,
        cache_keys,
        cache_values,
        w_output,
        w_eg,
        w_eu,
        w_ed,
        w_dg,
        w_du,
        w_dd,
    )


def solution(mesh):
    return jax.shard_map(
        local,
        mesh=mesh,
        in_specs=(
            P("ep", None),
            P("ep"),
            P(),
            P(None, "tp"),
            P(None, "tp"),
            P(None, "tp"),
            P("ep", None, "tp"),
            P("ep", None, "tp"),
            P("tp"),
            P("tp", None),
            P(),
            P(),
            P(),
            P(),
            P(),
            P("ep", None),
            P("ep", None, "tp"),
            P("ep", None, "tp"),
            P("ep", "tp", None),
            P(None, ("ep", "tp")),
            P(None, ("ep", "tp")),
            P(("ep", "tp"), None),
        ),
        out_specs=P("ep", "tp"),
        check_vma=False,
    )
```
